32 devices in a mesh: rep: 4 (over z), fs: 4 (over y, x), tp: 2 (over core).
Axes of the slice: x: 2, y: 2, z: 4, core: 2. Of those that a mesh axis runs over, the one named last changes fastest.
Arguments:
- pre_gate: bfloat16 [3072, 7936], P('rep', ('fs', 'tp')), may hold values from -6 to 6
- pre_up: bfloat16 [3072, 7936], P('rep', ('fs', 'tp')), may hold values from -6 to 6
- cotangent: bfloat16 [3072, 4096], P('rep', ('fs', 'tp')), may hold values from -6 to 6
- down_weight: bfloat16 [7936, 4096], P(('fs', 'tp')), may hold values from -0.0625 to 0.0625
Outputs:
- grad_gate: bfloat16 [3072, 7936], P('rep', ('fs', 'tp'))
- grad_up: bfloat16 [3072, 7936], P('rep', ('fs', 'tp'))
- grad_down: float32 [7936, 4096], P(('fs', 'tp'), 'rep')
- row_squares: float32 [7936], P(('fs', 'tp'))
The draws below stay inside these ranges and needn't reach their ends.
All inputs are finite; a program needn't handle non-finite values.
Results may differ from the reference program's by a relative error of at most 0.0034.
Values may be sent and summed in bfloat16 or wider, within the bound.
No kernel may reach another device: no remote copies, remote signals or barrier semaphores. Data moves between devices by JAX's collectives and lax.ppermute only.
A program may use at most 128 MiB of HBM per device.

```python
import jax
import jax.numpy as jnp

D = 4096
FF = 7936
TOKENS = 3072


def with_spikes(result, rng, source, target, shards_of, factor):
    def block_of(axis_at):
        return (jnp.arange(result.shape[axis_at]) // (result.shape[axis_at] // shards_of)).reshape((-1,) + (1,) * (result.ndim - 1 - axis_at))

    first = jax.random.permutation(rng, shards_of)[block_of(target)]
    other_side = (block_of(target) + shards_of // 2) % shards_of
    return jnp.where((block_of(source) == first) | (block_of(source) == other_side), factor * result, result)


def level_of(rng, extent, shards, low, top_value):
    def one(dim, blocks):
        steps = jax.random.uniform(jax.random.fold_in(jax.random.fold_in(rng, 6), dim), (blocks,), jnp.float32, low / len(shards), top_value / len(shards))
        return jnp.repeat(jnp.exp(steps), extent[dim] // blocks).reshape((-1,) + (1,) * (len(extent) - dim - 1))

    gain = one(*shards[0])
    for cut in shards[1:]:
        gain = gain * one(*cut)
    return gain


def normal_values(own_key, dims, scale, reach, shards=(), dtype=jnp.bfloat16):
    entries = scale * jax.random.normal(own_key, dims, jnp.float32)
    if shards:
        entries = entries * level_of(own_key, dims, shards, -0.22, 0.18)
    return jnp.clip(entries, -reach, reach).astype(dtype)


def bell_draw_with(stream_key, dims, spread, most, cuts, heavy, held_as=jnp.bfloat16):
    drawn = spread * jax.random.normal(stream_key, dims, jnp.float32)
    if cuts:
        drawn = drawn * level_of(stream_key, dims, cuts, -0.22, 0.18)
    return jnp.clip(with_spikes(drawn, jax.random.fold_in(stream_key, 3), *heavy), -most, most).astype(held_as)


def setup_inputs(seed: int = 0) -> dict:
    arg_keys = jax.random.split(jax.random.key(seed), 5)
    pre_gate = normal_values(arg_keys[0], (TOKENS, FF), 1.5, 6.0, ((0, 4), (1, 8)))
    pre_up = normal_values(arg_keys[1], (TOKENS, FF), 1.0, 6.0, ((0, 4), (1, 8)))
    cotangent = bell_draw_with(arg_keys[2], (TOKENS, D), 1.0, 6.0, ((0, 4), (1, 8)), (0, 1, 8, 2.0))
    down_weight = normal_values(arg_keys[3], (FF, D), FF ** -0.5, 0.0625, ((0, 8),))
    return dict(pre_gate=pre_gate, pre_up=pre_up, cotangent=cotangent, down_weight=down_weight)


def reference(pre_gate, pre_up, cotangent, down_weight):
    gate_wide = pre_gate.astype(jnp.float32)
    up_wide = pre_up.astype(jnp.float32)
    sigmoid_gate = jax.nn.sigmoid(gate_wide)
    act = gate_wide * sigmoid_gate
    hidden = (act * up_wide).astype(jnp.bfloat16)
    grad_hidden = jnp.dot(cotangent, down_weight.T, preferred_element_type=jnp.float32)
    grad_up = (grad_hidden * act).astype(jnp.bfloat16)
    slope = sigmoid_gate * (1.0 + gate_wide * (1.0 - sigmoid_gate))
    grad_gate = (grad_hidden * up_wide * slope).astype(jnp.bfloat16)
    grad_down = jnp.dot(hidden.T, cotangent, preferred_element_type=jnp.float32)
    row_squares = jnp.sum(grad_down * grad_down, axis=1)
    return grad_gate, grad_up, grad_down, row_squares
```

```python
import jax
import jax.numpy as jnp
from jax import lax
from jax.experimental import pallas as pl
from jax.experimental.pallas import tpu as pltpu
from jax.sharding import PartitionSpec as P


F32 = jnp.float32
BF16 = jnp.bfloat16


def dot(a, b, ca, cb):
    return lax.dot_general(
        a, b, (((ca,), (cb,)), ((), ())), preferred_element_type=F32
    )


def elementwise(pre_gate, pre_up):
    gate = pre_gate.astype(F32)
    up = pre_up.astype(F32)
    sig = jax.nn.sigmoid(gate)
    act = gate * sig
    slope = sig * (1.0 + gate * (1.0 - sig))
    return act, up, slope


def general(pre_gate, pre_up, cotangent, down_weight):
    act, up, slope = elementwise(pre_gate, pre_up)
    hidden = (act * up).astype(BF16)
    piece = lax.all_gather(cotangent, ("fs", "tp"), axis=1, tiled=True)
    grad = dot(piece, down_weight, 1, 1)
    block = dot(piece, hidden, 0, 0)
    grad_up = (grad * act).astype(BF16)
    grad_gate = (grad * up * slope).astype(BF16)
    grad_down = lax.psum_scatter(block, "rep", scatter_dimension=0, tiled=True).T
    squares = lax.psum(jnp.sum(grad_down * grad_down, axis=1), "rep")
    return grad_gate, grad_up, grad_down, squares


def products(hiddens, own, partner, far, flags):
    width, rows = hiddens[0].shape
    block = own[0].shape[1]
    half = rows // 2

    def kernel(flags_ref, *refs):
        h_own, h_partner, h_far = refs[:3]
        own_refs, partner_refs, far_refs = refs[3:7], refs[7:15], refs[15:23]
        mate_ref, z_ref = refs[23:]
        near = pl.multiple_of(flags_ref[2], half)
        other = pl.multiple_of(half - flags_ref[2], half)

        def mul(a, b):
            return jnp.dot(a, b, preferred_element_type=F32)

        for core in range(2):
            column = pl.multiple_of((flags_ref[1] ^ core) * block, block)
            for at_x in range(2):
                total = mul(h_own[...], own_refs[2 * core + at_x][...])
                for h, group in ((h_partner, partner_refs), (h_far, far_refs)):
                    a, b = group[4 * core + at_x], group[4 * core + 2 + at_x]
                    total += mul(h[:, pl.ds(near, half)], a[...])
                    total += mul(h[:, pl.ds(other, half)], b[...])
                is_z = flags_ref[0] == 1 - at_x

                @pl.when(is_z)
                def _(total=total, column=column):
                    z_ref[:, pl.ds(column, block)] = total

                @pl.when(jnp.logical_not(is_z))
                def _(total=total, column=column):
                    mate_ref[:, pl.ds(column, block)] = total.astype(BF16)

    vmem = pl.BlockSpec(memory_space=pltpu.VMEM)
    flops = 2 * 3 * rows * width * 4 * block
    return pl.pallas_call(
        kernel,
        in_specs=[pl.BlockSpec(memory_space=pltpu.SMEM)] + [vmem] * 23,
        out_specs=[vmem, vmem],
        out_shape=[
            jax.ShapeDtypeStruct((width, 2 * block), BF16),
            jax.ShapeDtypeStruct((width, 2 * block), F32),
        ],
        cost_estimate=pl.CostEstimate(
            flops=flops, bytes_accessed=rows * block * 24, transcendentals=0
        ),
        name="products",
    )(flags, *hiddens, *own, *partner, *far)


def line(pre_gate, pre_up, shard, down_weight):
    z = lax.axis_index("rep")
    fs = lax.axis_index("fs")
    t = lax.axis_index("tp")
    y, x = fs >> 1, fs & 1
    rows = shard.shape[0]
    ff = pre_gate.shape[1]
    r2 = rows // 2
    own_half = z >> 1
    holds = y == own_half
    x_is_z = x == (z & 1)
    tie = lax.optimization_barrier

    def square(v, flip, who=lambda a, b: True):
        pairs = [
            (4 * a + b, 4 * a + (b ^ flip))
            for a in range(4)
            for b in range(4)
            if who(a, b)
        ]
        return lax.ppermute(v, ("rep", "fs"), pairs)

    def holder(a, b):
        return b >> 1 == a >> 1

    def other(a, b):
        return not holder(a, b)

    def to_t(v):
        return lax.ppermute(v, "tp", [(0, 1), (1, 0)])

    def to_partner(v):
        return lax.ppermute(v, "rep", [(1, 2), (2, 1)])

    def to_far(v):
        return lax.ppermute(v, "rep", [(0, 2), (3, 1)])

    def to_mate(v):
        return lax.ppermute(v, "rep", [(i, i ^ 1) for i in range(4)])

    def pair(first, a, b, axis):
        return jnp.concatenate(
            [jnp.where(first, a, b), jnp.where(first, b, a)], axis=axis
        )

    spans, start = [], 0
    for size in SPANS:
        stop = min(start + size, ff)
        if stop > start:
            spans.append((start, stop))
        start = stop

    top, bottom = shard[:r2], shard[r2:]
    yn_a = square(tie(top), 2, other)
    ys = square(shard, 2, holder)
    xn = square(shard, 1, holder)
    yo = square(shard, 2, other)
    cross = tie(jnp.where(holds, yn_a, bottom))

    parts = []
    for a, b in spans:
        gate, up = pre_gate[:, a:b].astype(F32), pre_up[:, a:b].astype(F32)
        parts.append(tie((gate * jax.nn.sigmoid(gate) * up).astype(BF16).T))
    h_partner = [to_partner(part) for part in parts]
    h_far = [to_far(part) for part in parts]
    q_partner = to_partner(cross)
    q_far = to_far(cross)

    yx = square(xn, 2, holder)
    ys, xn, yx, s1 = tie((ys, xn, yx, shard))
    own_x = jnp.where(holds, s1, ys)
    own_xn = jnp.where(holds, xn, yx)
    own_x, own_xn = tie((own_x, own_xn))
    own = (own_x, own_xn, to_t(own_x), to_t(own_xn))

    def spread(q, last):
        qx, qy = square(q, 1), square(q, 2)
        qd = square(qx if last == 2 else qy, last)
        four = (q, qx, qy, qd)
        return (*four, *[to_t(v) for v in four])

    partner, far = spread(q_partner, 1), spread(q_far, 2)
    flags = jnp.stack([x_is_z.astype(jnp.int32), t, jnp.where(holds, r2, 0)])

    yo, s2 = tie((yo, shard))
    oth_x = tie(jnp.where(holds, yo, s2))
    oth_xn = square(oth_x, 1)
    own_t, oth_t = own[2:], (to_t(oth_x), to_t(oth_xn))

    def columns(blocks, blocks_t):
        here = pair(t == 0, blocks[0], blocks_t[0], 1)
        there = pair(t == 0, blocks[1], blocks_t[1], 1)
        return pair(x == 0, here, there, 1)

    full = pair(
        own_half == 0, columns(own[:2], own_t), columns((oth_x, oth_xn), oth_t), 1
    )
    act, up, slope = elementwise(*tie((pre_gate, pre_up, full))[:2])
    grad = dot(full, down_weight, 1, 1)
    grad_up = (grad * act).astype(BF16)
    grad_gate = (grad * up * slope).astype(BF16)

    zs, backs = [], []
    for k in range(len(parts)):
        hiddens = (parts[k], h_partner[k], h_far[k])
        if k == len(parts) - 1:
            part, grad_up, grad_gate = tie((parts[k], grad_up, grad_gate))
            hiddens = (part, *hiddens[1:])
        mate_sum, own_sum = products(hiddens, own, partner, far, flags)
        backs.append(to_mate(mate_sum))
        zs.append(own_sum)
    downs, squares = [], []
    for own_sum, back in zip(zs, backs):
        down = own_sum + back.astype(F32)
        downs.append(down)
        squares.append(jnp.sum(down * down, axis=1))
    partial = jnp.concatenate(squares, axis=0)
    total = partial
    for shift in (1, 2, 3):
        total = total + lax.ppermute(
            partial, "rep", [(i, (i + shift) % 4) for i in range(4)]
        )
    return grad_gate, grad_up, jnp.concatenate(downs, axis=0), total


SPANS = (384, 384, 384)


def solution(mesh):
    sizes = dict(mesh.shape)
    placed = P("rep", ("fs", "tp"))

    def shard_mapped(body):
        return jax.shard_map(
            body,
            mesh=mesh,
            in_specs=(placed, placed, placed, P(("fs", "tp"), None)),
            out_specs=(placed, placed, P(("fs", "tp"), "rep"), P(("fs", "tp"))),
            check_vma=False,
        )

    if (sizes["rep"], sizes["fs"], sizes["tp"]) != (4, 4, 2):
        return shard_mapped(general)

    return shard_mapped(line)
```
